32 devices in a mesh: sp: 16 (over z, y, x), tp: 2 (over core).
Axes of the slice: x: 2, y: 2, z: 4, core: 2. Of those that a mesh axis runs over, the one named last changes fastest.
Arguments:
- tokens: bfloat16 [2, 4096, 2048], P(None, 'sp'), may hold values from -6 to 6
- key_weight: bfloat16 [2048, 2048], P(None, 'tp'), may hold values from -0.125 to 0.125
- value_weight: bfloat16 [2048, 2048], P(None, 'tp'), may hold values from -0.125 to 0.125
- cum_gate: float32 [2, 4096, 32], P(None, 'sp', 'tp'), may hold values from -493.64 to 0, as said below
- new_input: bfloat16 [2, 2048], replicated, may hold values from -6 to 6
- new_query: bfloat16 [2, 2048], P(None, 'tp'), may hold values from -360 to 360
- new_gate: float32 [2, 32], P(None, 'tp'), may hold values from -493.64 to 0
- out_weight: bfloat16 [2048, 2048], P('tp', 'sp'), may hold values from -0.75 to 0.75
Outputs:
- key_cache: bfloat16 [2, 16, 256, 2048], P(None, 'sp', None, 'tp')
- value_cache: bfloat16 [2, 16, 256, 2048], P(None, 'sp', None, 'tp')
- gate_cache: float32 [2, 16, 256, 32], P(None, 'sp', None, 'tp')
- mixed: bfloat16 [2, 2048], P(None, 'sp')
The draws below stay inside these ranges and needn't reach their ends.
Inputs may be any that keep to these rules, and one draw needn't show every extreme that they name: For each sequence and head cum_gate does not rise along positions, and new_gate lies at or below the value at the last cached position.
All inputs are finite; a program needn't handle non-finite values.
Results may differ from the reference program's by a relative error of at most 0.015.
Values may be sent and summed in bfloat16 or wider, within the bound.
A program may use at most 64 MiB of HBM per device.

```python
import math
import jax
import jax.numpy as jnp
from jax import lax

D = 2048
ATTENTION_HEADS = 32
HEAD_DIM = 64
BATCH_SEQUENCES = 2
SPAN = 256
CACHED_LENGTH = 4096
N_SP = 16
N_TP = 2


def gate_logs(key):
    head_order = jax.random.permutation(jax.random.fold_in(key, 1), ATTENTION_HEADS)
    lagging_heads = head_order < ATTENTION_HEADS // 2
    fast_rate = jnp.exp(jax.random.uniform(jax.random.fold_in(key, 2), (ATTENTION_HEADS,), jnp.float32, math.log(0.01), math.log(1.0 / 30.0)))
    slow_rate = jax.random.uniform(jax.random.fold_in(key, 3), (ATTENTION_HEADS,), jnp.float32, 0.2, 0.6) / (CACHED_LENGTH + 1)
    decay_rate = jnp.where(lagging_heads, slow_rate, fast_rate)
    block_count = CACHED_LENGTH // SPAN
    decay_factor = jnp.exp(jax.random.uniform(jax.random.fold_in(key, 4), (BATCH_SEQUENCES, block_count, 1, ATTENTION_HEADS), jnp.float32, math.log(0.5), math.log(2.0)))
    decay_factor = jnp.broadcast_to(decay_factor, (BATCH_SEQUENCES, block_count, SPAN, ATTENTION_HEADS)).reshape(BATCH_SEQUENCES, CACHED_LENGTH, ATTENTION_HEADS)
    decay_factor = jnp.concatenate([decay_factor, jnp.ones((BATCH_SEQUENCES, 1, ATTENTION_HEADS), jnp.float32)], axis=1)
    random_jitter = jax.random.uniform(jax.random.fold_in(key, 5), (BATCH_SEQUENCES, CACHED_LENGTH + 1, ATTENTION_HEADS), jnp.float32, 0.3, 1.7)
    spike_positions = jax.random.randint(jax.random.fold_in(key, 6), (BATCH_SEQUENCES, 2, ATTENTION_HEADS), 0, CACHED_LENGTH + 1)
    position_index = jnp.arange(CACHED_LENGTH + 1, dtype=jnp.int32)
    spike_count = jnp.sum((position_index[None, :, None, None] == spike_positions[:, None, :, :]).astype(jnp.float32), axis=2)
    spike_height = jax.random.uniform(jax.random.fold_in(key, 7), (BATCH_SEQUENCES, CACHED_LENGTH + 1, ATTENTION_HEADS), jnp.float32, 0.22, 0.69)
    forget_logits = -decay_rate * decay_factor * random_jitter - spike_count * spike_height * lagging_heads.astype(jnp.float32)
    return jnp.cumsum(forget_logits, axis=1)


def draw_cum_gate(key, part):
    return gate_logs(key)[:, :CACHED_LENGTH, :]


def draw_new_gate(key, part):
    return gate_logs(key)[:, CACHED_LENGTH, :]


def draw_new_query(key, part):
    query_base = jax.random.truncated_normal(jax.random.fold_in(key, 21), -6.0, 6.0, (BATCH_SEQUENCES, D), jnp.float32)
    return query_base.astype(jnp.bfloat16)


def level_of(key, extent, cuts, low, high):
    gain = 1.0
    for axis_at, blocks in cuts:
        draws = jax.random.uniform(jax.random.fold_in(jax.random.fold_in(key, 6), axis_at), (blocks,), jnp.float32, low / len(cuts), high / len(cuts))
        gain = gain * jnp.repeat(jnp.exp(draws), extent[axis_at] // blocks).reshape((-1,) + (1,) * (len(extent) - 1 - axis_at))
    return gain


def scatter_about(own_key, shape, scale, limit, cuts=(), held_as=jnp.bfloat16):
    drawn = scale * jax.random.normal(own_key, shape, jnp.float32)
    if cuts:
        drawn = drawn * level_of(own_key, shape, cuts, -0.22, 0.18)
    return jnp.clip(drawn, -limit, limit).astype(held_as)


def setup_inputs(seed: int = 0) -> dict:
    streams_of = jax.random.split(jax.random.key(seed), 9)
    return {
        "tokens": scatter_about(streams_of[0], (BATCH_SEQUENCES, CACHED_LENGTH, D), 1.0, 6.0, ((1, 16),)),
        "key_weight": scatter_about(streams_of[1], (D, D), D ** -0.5, 0.125, ((1, 2),)),
        "value_weight": scatter_about(streams_of[2], (D, D), D ** -0.5, 0.125, ((1, 2),)),
        "cum_gate": draw_cum_gate(jax.random.fold_in(streams_of[8], 71), 0),
        "new_input": scatter_about(streams_of[4], (BATCH_SEQUENCES, D), 1.0, 6.0),
        "new_query": draw_new_query(jax.random.fold_in(streams_of[8], 71), 0),
        "new_gate": draw_new_gate(jax.random.fold_in(streams_of[8], 71), 0),
        "out_weight": scatter_about(streams_of[7], (D, D), HEAD_DIM ** -0.5, 0.75, ((0, 2), (1, 16))),
    }


def cyclic(rows):
    shaped = rows.reshape(rows.shape[0], SPAN, N_SP, rows.shape[2])
    return jnp.transpose(shaped, (0, 2, 1, 3))


def read_one(inputs):
    key_rows, value_rows, gate_rows, query_row, gate_now, key_now, value_now = inputs
    score_scale = HEAD_DIM ** -0.5
    key_heads = key_rows.reshape(N_SP, SPAN, ATTENTION_HEADS, HEAD_DIM).astype(jnp.float32)
    value_heads = value_rows.reshape(N_SP, SPAN, ATTENTION_HEADS, HEAD_DIM).astype(jnp.float32)
    query_heads = query_row.reshape(ATTENTION_HEADS, HEAD_DIM).astype(jnp.float32)
    scores = jnp.einsum("hd,rlhd->hrl", query_heads, key_heads) * score_scale
    scores = scores + gate_now[:, None, None] - jnp.transpose(gate_rows, (2, 0, 1))
    class_top = jnp.max(scores, axis=2)
    expo = jnp.exp(scores - class_top[:, :, None])
    class_total = jnp.sum(expo, axis=2)
    rounded = expo.astype(jnp.bfloat16).astype(jnp.float32)
    class_num = jnp.einsum("hrl,rlhd->hrd", rounded, value_heads)
    cached_top = jnp.max(class_top, axis=1)
    weight = jnp.exp(class_top - cached_top[:, None])
    cached_total = jnp.sum(weight * class_total, axis=1)
    cached_num = jnp.sum(weight[:, :, None] * class_num, axis=1)
    own_score = jnp.sum(query_heads * key_now.reshape(ATTENTION_HEADS, HEAD_DIM).astype(jnp.float32), axis=1) * score_scale
    highest = jnp.maximum(cached_top, own_score)
    keep = jnp.exp(cached_top - highest)
    own_expo = jnp.exp(own_score - highest)
    totals = cached_total * keep + own_expo
    own_rounded = lax.optimization_barrier(own_expo.astype(jnp.bfloat16)).astype(jnp.float32)
    numerator = cached_num * keep[:, None] + own_rounded[:, None] * value_now.reshape(ATTENTION_HEADS, HEAD_DIM).astype(jnp.float32)
    return (numerator / totals[:, None]).astype(jnp.bfloat16).reshape(ATTENTION_HEADS * HEAD_DIM)


def reference(tokens, key_weight, value_weight, cum_gate, new_input, new_query, new_gate, out_weight):
    batch_rows, length, width = tokens.shape
    flat_rows = tokens.reshape(batch_rows * length, width)
    keys = jnp.dot(flat_rows, key_weight, preferred_element_type=jnp.float32).astype(jnp.bfloat16).reshape(batch_rows, length, width)
    values = jnp.dot(flat_rows, value_weight, preferred_element_type=jnp.float32).astype(jnp.bfloat16).reshape(batch_rows, length, width)
    key_cache = cyclic(keys)
    value_cache = cyclic(values)
    gate_cache = cyclic(cum_gate)
    key_now = jnp.dot(new_input, key_weight, preferred_element_type=jnp.float32).astype(jnp.bfloat16)
    value_now = jnp.dot(new_input, value_weight, preferred_element_type=jnp.float32).astype(jnp.bfloat16)
    attended = lax.map(read_one, (key_cache, value_cache, gate_cache, new_query, new_gate, key_now, value_now))
    grouped = attended.reshape(BATCH_SEQUENCES, N_TP, D // N_TP).astype(jnp.float32)
    weight_groups = out_weight.reshape(N_TP, D // N_TP, D).astype(jnp.float32)
    partial_value = jnp.einsum("bgk,gkn->gbn", grouped, weight_groups)
    partial_value = lax.optimization_barrier(partial_value.astype(jnp.bfloat16)).astype(jnp.float32)
    mixed = jnp.sum(partial_value, axis=0).astype(jnp.bfloat16)
    return (key_cache, value_cache, gate_cache, mixed)
```

```python
import functools
import jax
import jax.numpy as jnp
from jax import lax
from jax.experimental import pallas as pl
from jax.experimental.pallas import tpu as pltpu
from jax.sharding import PartitionSpec as P

MESH = pl.DeviceIdType.MESH
F32 = jnp.float32
BF16 = jnp.bfloat16
EXACT = lax.Precision.HIGHEST
GROUPS = 4
TILE = 256


def joined(value, axis, join):
    pieces = jax.tree.map(lambda part: lax.all_gather(part, axis), value)
    head = jax.tree.map(lambda part: part[0], pieces)
    tail = jax.tree.map(lambda part: part[1:], pieces)
    running, _ = lax.scan(lambda running, share: (join(running, share), None), head, tail)
    return running


def combine_parts(first, second):
    highest = jnp.maximum(first[0], second[0])
    first_scale = jnp.exp(first[0] - highest)
    second_scale = jnp.exp(second[0] - highest)
    total = first[1] * first_scale + second[1] * second_scale
    numer = first[2] * first_scale[:, :, None] + second[2] * second_scale[:, :, None]
    return (highest, total, numer)


def plain_body(tokens, key_weight, value_weight, cum_gate, new_input, new_query, new_gate, out_weight):
    local_width = key_weight.shape[1]
    parts = lax.axis_size("sp")
    seq_count, span, width = tokens.shape
    per_peer = span // parts
    flat_rows = tokens.reshape(seq_count * span, width)
    key_local = jnp.dot(flat_rows, key_weight, preferred_element_type=jnp.float32).astype(
        jnp.bfloat16
    )
    value_local = jnp.dot(flat_rows, value_weight, preferred_element_type=jnp.float32).astype(
        jnp.bfloat16
    )
    shaped = (seq_count, per_peer, parts, local_width)
    key_moved, value_moved = (
        lax.all_to_all(key_local.reshape(shaped), "sp", split_axis=2, concat_axis=1, tiled=True),
        lax.all_to_all(value_local.reshape(shaped), "sp", split_axis=2, concat_axis=1, tiled=True),
    )
    key_cache = key_moved.reshape(seq_count, 1, span, local_width)
    value_cache = value_moved.reshape(seq_count, 1, span, local_width)
    head_count = cum_gate.shape[2]
    gate_shaped = cum_gate.reshape(seq_count, per_peer, parts, head_count)
    gate_cache = lax.all_to_all(gate_shaped, "sp", split_axis=2, concat_axis=1, tiled=True).reshape(
        seq_count, 1, span, head_count
    )
    head_size = local_width // head_count
    score_scale = head_size ** (-0.5)
    key_now = jnp.dot(new_input, key_weight, preferred_element_type=jnp.float32).astype(
        jnp.bfloat16
    )
    value_now = jnp.dot(new_input, value_weight, preferred_element_type=jnp.float32).astype(
        jnp.bfloat16
    )
    key_now = key_now.reshape(seq_count, head_count, head_size)
    value_now = value_now.reshape(seq_count, head_count, head_size)
    query_heads = new_query.reshape(seq_count, head_count, head_size)
    key_heads = key_cache.reshape(seq_count, span, head_count, head_size)
    value_heads = value_cache.reshape(seq_count, span, head_count, head_size)
    scores = (
        jnp.einsum("nhd,nlhd->nhl", query_heads, key_heads, preferred_element_type=jnp.float32)
        * score_scale
    )
    scores = (
        scores
        + new_gate[:, :, None]
        - jnp.swapaxes(gate_cache.reshape(seq_count, span, head_count), 1, 2)
    )
    class_top = jnp.max(scores, axis=2)
    expo = jnp.exp(scores - class_top[:, :, None])
    class_total = jnp.sum(expo, axis=2)
    class_num = jnp.einsum(
        "nhl,nlhd->nhd", expo.astype(jnp.bfloat16), value_heads, preferred_element_type=jnp.float32
    )
    cached_top, cached_total, cached_num = joined(
        (class_top, class_total, class_num), "sp", combine_parts
    )
    own_score = (
        jnp.einsum("nhd,nhd->nh", query_heads, key_now, preferred_element_type=jnp.float32)
        * score_scale
    )
    highest = jnp.maximum(cached_top, own_score)
    keep = jnp.exp(cached_top - highest)
    own_expo = jnp.exp(own_score - highest)
    totals = cached_total * keep + own_expo
    own_rounded = lax.optimization_barrier(own_expo.astype(jnp.bfloat16)).astype(jnp.float32)
    numerator = cached_num * keep[:, :, None] + own_rounded[:, :, None] * value_now.astype(
        jnp.float32
    )
    attended = (numerator / totals[:, :, None]).astype(jnp.bfloat16).reshape(seq_count, local_width)
    partial_value = jnp.dot(attended, out_weight, preferred_element_type=jnp.float32)
    partial_value = lax.optimization_barrier(partial_value.astype(jnp.bfloat16)).astype(jnp.float32)
    mixed = lax.psum(partial_value.astype(jnp.bfloat16), "tp")
    return (key_cache, value_cache, gate_cache, mixed)


def iota(shape, axis):
    return lax.broadcasted_iota(jnp.int32, shape, axis)


def dot(a, b, contract=((1,), (0,)), precision=None):
    return lax.dot_general(
        a, b, (contract, ((), ())), precision=precision, preferred_element_type=F32
    )


def one_hot(condition, dtype):
    return jnp.where(condition, 1.0, 0.0).astype(dtype)


def kernel(
    n, m, heads, head_size,
    tokens_ref, wk_ref, wv_ref, gate_ref, input_ref, query_ref, newgate_ref, ow_ref,
    kc_ref, vc_ref, gc_ref, mixed_ref,
    tok, wk, wv, ow, psend, recv, kst, vst, gsend, grecv, qblk, scores, expo,
    know, vnow, stat, statall, num, numall, coef, xsend, xrecv,
    load_sem, own_sem, out_sem, tok_ss, tok_rs, fwd_ss, fwd_rs, gate_ss, gate_rs,
    stat_ss, stat_rs, num_ss, num_rs, x_ss, x_rs,
):
    me = lax.axis_index("sp")
    t = lax.axis_index("tp")
    other = 1 - t
    seqs, span, width = tokens_ref.shape
    local = wk_ref.shape[1]
    tiles = local // TILE
    per_group = n // GROUPS
    log_m = m.bit_length() - 1
    log_hd = head_size.bit_length() - 1
    scale = head_size ** (-0.5)

    loads = [
        pltpu.make_async_copy(tokens_ref.at[t], tok.at[t], load_sem.at[0]),
        pltpu.make_async_copy(tokens_ref.at[other], tok.at[other], load_sem.at[1]),
        pltpu.make_async_copy(wk_ref, wk, load_sem.at[2]),
        pltpu.make_async_copy(wv_ref, wv, load_sem.at[3]),
        pltpu.make_async_copy(ow_ref, ow, load_sem.at[4]),
    ]
    for load in loads:
        load.start()

    barrier = pltpu.get_barrier_semaphore()

    def greet(k, carry):
        pl.semaphore_signal(
            barrier, inc=1, device_id=(lax.rem(me + k, n), t), device_id_type=MESH
        )
        return carry

    lax.fori_loop(1, n, greet, 0)
    pl.semaphore_signal(barrier, inc=1, device_id=(me, other), device_id_type=MESH)

    quarter = m // 4
    stacked = jnp.concatenate([gate_ref[...]] * 4, axis=0)
    row = iota((span, span), 0)
    col = iota((span, span), 1)
    block_rows = n * quarter
    log_q = quarter.bit_length() - 1
    step_q = row >> (block_rows.bit_length() - 1)
    inner = row & (block_rows - 1)
    place = (step_q * quarter + (inner & (quarter - 1))) * n + (inner >> log_q)
    moved_gate = dot(one_hot(col == place, F32), stacked, ((1,), (1,)), EXACT)
    lanes = seqs * heads
    keep_lane = (iota(moved_gate.shape, 1) // lanes) == (
        iota(moved_gate.shape, 0) >> (block_rows.bit_length() - 1)
    )
    moved_gate = jnp.where(keep_lane, moved_gate, 0.0)
    packed = moved_gate[0:block_rows]
    for q in range(1, 4):
        packed = packed + moved_gate[q * block_rows : (q + 1) * block_rows]
    for r in range(n):
        gsend[r] = packed[r * quarter : (r + 1) * quarter]

    loads[0].wait()
    perm = one_hot(col == (row & (m - 1)) * n + (row >> log_m), BF16)
    for j in range(width // 512):
        cols = slice(j * 512, (j + 1) * 512)
        psend[:, :, cols] = dot(perm, tok[t, :, cols]).astype(BF16).reshape(n, m, 512)

    head_of = iota((heads, local), 1) >> log_hd
    mine = head_of == iota((heads, local), 0)
    for b in range(seqs):
        qblk[b * heads : (b + 1) * heads] = jnp.where(
            mine, query_ref[b : b + 1, :].astype(F32), 0.0
        ).astype(BF16)
    scores[...] = jnp.zeros_like(scores)

    pl.semaphore_wait(barrier, n)

    def peer(k):
        far = lax.div(k, per_group)
        near = lax.rem(k, per_group)
        zone = lax.rem(lax.div(me, per_group) + far, GROUPS)
        return zone * per_group + lax.rem(lax.rem(me, per_group) + near, per_group)

    def tok_copy(k, to, source):
        return pltpu.make_async_remote_copy(
            src_ref=psend.at[to], dst_ref=recv.at[t, source],
            send_sem=tok_ss.at[k], recv_sem=tok_rs.at[source],
            device_id=(to, t), device_id_type=MESH,
        )

    def gate_copy(k, to, source):
        return pltpu.make_async_remote_copy(
            src_ref=gsend.at[to], dst_ref=grecv.at[source],
            send_sem=gate_ss.at[k], recv_sem=gate_rs.at[source],
            device_id=(to, t), device_id_type=MESH,
        )

    def stat_copy(k, to, source):
        return pltpu.make_async_remote_copy(
            src_ref=stat, dst_ref=statall.at[source],
            send_sem=stat_ss.at[k], recv_sem=stat_rs.at[source],
            device_id=(to, t), device_id_type=MESH,
        )

    def num_copy(k, to, source):
        return pltpu.make_async_remote_copy(
            src_ref=num, dst_ref=numall.at[source],
            send_sem=num_ss.at[k], recv_sem=num_rs.at[source],
            device_id=(to, t), device_id_type=MESH,
        )

    def forward(held, source, target_batch):
        return pltpu.make_async_remote_copy(
            src_ref=held, dst_ref=recv.at[target_batch, source],
            send_sem=fwd_ss.at[source], recv_sem=fwd_rs.at[source],
            device_id=(me, other), device_id_type=MESH,
        )

    def send_tokens(k, carry):
        tok_copy(k, peer(k), me).start()
        return carry

    def send_gates(k, carry):
        gate_copy(k, peer(k), me).start()
        return carry

    lax.fori_loop(1, n, send_gates, 0)
    for lo, hi in SEND_ORDER(per_group):
        lax.fori_loop(lo, hi, send_tokens, 0)
    own_copy = pltpu.make_async_copy(psend.at[me], recv.at[t, me], own_sem)
    own_copy.start()
    forward(psend.at[me], me, t).start()

    loads[1].wait()
    loads[2].wait()

    def key_tile(j, carry):
        cols = pl.ds(pl.multiple_of(j * TILE, TILE), TILE)
        weight = wk[:, cols]
        know[:, cols] = dot(input_ref[...], weight).astype(BF16).astype(F32)
        for b in range(seqs):
            keys = dot(tok[b], weight).astype(BF16)
            rows = slice(b * heads, (b + 1) * heads)
            scores[rows] += dot(qblk[rows, cols], keys, ((1,), (1,)))
        return carry

    lax.fori_loop(0, tiles, key_tile, 0)

    eye = iota((heads, heads), 0) == iota((heads, heads), 1)
    eye_wide = iota((heads, 128), 0) == iota((heads, 128), 1)
    for b in range(seqs):
        rows = slice(b * heads, (b + 1) * heads)
        lift = jnp.sum(jnp.where(eye, newgate_ref[b : b + 1, :], 0.0), axis=1, keepdims=True)
        score = scores[rows] * scale + lift - gate_ref[rows]
        top = jnp.max(score, axis=1, keepdims=True)
        weights = jnp.exp(score - top)
        total = jnp.sum(weights, axis=1, keepdims=True)
        expo[rows] = weights.astype(BF16)
        stat[b : b + 1, :] = jnp.sum(jnp.where(eye_wide, top, 0.0), axis=0, keepdims=True)
        stat[seqs + b : seqs + b + 1, :] = jnp.sum(
            jnp.where(eye_wide, total, 0.0), axis=0, keepdims=True
        )

    loads[3].wait()

    def value_tile(j, carry):
        cols = pl.ds(pl.multiple_of(j * TILE, TILE), TILE)
        weight = wv[:, cols]
        vnow[:, cols] = dot(input_ref[...], weight).astype(BF16).astype(F32)
        held = (iota((heads, TILE), 1) >> log_hd) + j * (TILE // head_size)
        ours = held == iota((heads, TILE), 0)
        sums = []
        for b in range(seqs):
            values = dot(tok[b], weight).astype(BF16)
            full = dot(expo[b * heads : (b + 1) * heads], values)
            sums.append(jnp.sum(jnp.where(ours, full, 0.0), axis=0, keepdims=True))
        num[:, cols] = jnp.concatenate(sums, axis=0).astype(BF16)
        return carry

    lax.fori_loop(0, tiles, value_tile, 0)

    def send_read(k, carry):
        stat_copy(k, peer(k), me).start()
        num_copy(k, peer(k), me).start()
        return carry

    statall[me] = stat[...]
    numall[me] = num[...]
    lax.fori_loop(1, n, send_read, 0)

    def out_copies(zone):
        rows = pl.ds(pl.multiple_of(zone * per_group * m, per_group * m), per_group * m)
        return (
            pltpu.make_async_copy(kst.at[:, rows], kc_ref.at[:, rows], out_sem.at[0, zone]),
            pltpu.make_async_copy(vst.at[:, rows], vc_ref.at[:, rows], out_sem.at[1, zone]),
        )

    def pass_on(far, near_from):
        def step(near, carry):
            source = peer(far * per_group + near)
            tok_copy(0, source, source).wait_recv()
            forward(recv.at[t, source], source, t).start()
            return carry

        lax.fori_loop(near_from, per_group, step, 0)

    def project(far):
        zone = lax.rem(lax.div(me, per_group) + far, GROUPS)
        start = zone * per_group

        def arrived(near, carry):
            forward(recv.at[other, start + near], start + near, other).wait_recv()
            return carry

        lax.fori_loop(0, per_group, arrived, 0)
        rows = pl.ds(pl.multiple_of(start * m, per_group * m), per_group * m)

        def tile(j, carry):
            cols = pl.ds(pl.multiple_of(j * TILE, TILE), TILE)
            block = recv[:, pl.ds(start, per_group)].reshape(seqs * per_group * m, width)
            made = dot(block, wk[:, cols]).astype(BF16)
            kst[:, rows, cols] = made.reshape(seqs, per_group * m, TILE)
            made = dot(block, wv[:, cols]).astype(BF16)
            vst[:, rows, cols] = made.reshape(seqs, per_group * m, TILE)
            return carry

        lax.fori_loop(0, tiles, tile, 0)
        for copy in out_copies(zone):
            copy.start()

    def finish_gates():
        def arrived(k, carry):
            source = peer(k)
            gate_copy(k, source, source).wait_recv()
            return carry

        lax.fori_loop(1, n, arrived, 0)
        grecv[me] = gsend[me]
        held = jnp.concatenate([grecv[s] for s in range(n)], axis=0)
        place_row = iota((block_rows, span), 0)
        target = ((place_row >> log_q) << log_m) + (place_row & (quarter - 1))
        spot = iota((block_rows, span), 1)
        result = None
        for q in range(4):
            part = dot(held, one_hot(spot == target + q * quarter, F32), ((0,), (0,)), EXACT)
            part = part[q * lanes : (q + 1) * lanes]
            result = part if result is None else result + part
        gc_ref[...] = result

    def finish_read():
        def arrived(k, carry):
            source = peer(k)
            stat_copy(k, source, source).wait_recv()
            num_copy(k, source, source).wait_recv()
            return carry

        lax.fori_loop(1, n, arrived, 0)
        loads[4].wait()
        widen = one_hot((iota((128, local), 1) >> log_hd) == iota((128, local), 0), F32)
        own = dot(query_ref[...].astype(F32) * know[...], widen, ((1,), (1,)), EXACT) * scale
        numbers = numall[...].astype(F32)
        attended = []
        for b in range(seqs):
            tops = statall[:, b, :]
            totals = statall[:, seqs + b, :]
            cached_top = jnp.max(tops, axis=0, keepdims=True)
            weight = jnp.exp(tops - cached_top)
            cached_total = jnp.sum(weight * totals, axis=0, keepdims=True)
            own_score = own[b : b + 1]
            highest = jnp.maximum(cached_top, own_score)
            keep = jnp.exp(cached_top - highest)
            own_expo = jnp.exp(own_score - highest)
            total = cached_total * keep + own_expo
            coef[0:n] = weight * (keep / total)
            coef[n : n + 8] = jnp.broadcast_to(own_expo.astype(BF16).astype(F32) / total, (8, 128))
            wide = dot(coef[...], widen, precision=EXACT)
            cached = jnp.sum(numbers[:, b, :] * wide[0:n], axis=0, keepdims=True)
            attended.append(cached + vnow[b : b + 1, :] * wide[n : n + 1])
        attended = jnp.concatenate(attended, axis=0).astype(BF16)
        xsend[...] = dot(attended, ow[...]).astype(BF16)

    own_copy.wait()
    pass_on(0, 1)
    finish_gates()
    project(0)
    for far in FAR_ORDER[:-1]:
        pass_on(far, 0)
        project(far)
    finish_read()
    swap = pltpu.make_async_remote_copy(
        src_ref=xsend, dst_ref=xrecv, send_sem=x_ss, recv_sem=x_rs,
        device_id=(me, other), device_id_type=MESH,
    )
    swap.start()
    pass_on(FAR_ORDER[-1], 0)
    project(FAR_ORDER[-1])
    swap.wait()
    mixed_ref[...] = (xsend[...].astype(F32) + xrecv[...].astype(F32)).astype(BF16)

    def sent(k, carry):
        to = peer(k)
        tok_copy(k, to, me).wait_send()
        gate_copy(k, to, me).wait_send()
        stat_copy(k, to, me).wait_send()
        num_copy(k, to, me).wait_send()
        return carry

    lax.fori_loop(1, n, sent, 0)

    def passed(source, carry):
        forward(recv.at[t, source], source, t).wait_send()
        return carry

    lax.fori_loop(0, n, passed, 0)
    for zone in range(GROUPS):
        for copy in out_copies(zone):
            copy.wait()


FAR_ORDER = (1, 3, 2)


def SEND_ORDER(per_group):
    order = [(far * per_group, (far + 1) * per_group) for far in (2, 1, 3)]
    return order + [(1, per_group)]


def body(tokens, key_weight, value_weight, cum_gate, new_input, new_query, new_gate, out_weight):
    n = lax.axis_size("sp")
    seqs, span, width = tokens.shape
    local = key_weight.shape[1]
    heads = cum_gate.shape[2]
    head_size = local // heads
    m = span // n
    out_cols = out_weight.shape[1]
    gates = jnp.swapaxes(cum_gate, 1, 2).reshape(seqs * heads, span)
    anywhere = pl.BlockSpec(memory_space=pl.ANY)
    inside = pl.BlockSpec(memory_space=pltpu.VMEM)
    dma = pltpu.SemaphoreType.DMA
    key_cache, value_cache, gate_cache, mixed = pl.pallas_call(
        functools.partial(kernel, n, m, heads, head_size),
        out_shape=(
            jax.ShapeDtypeStruct((seqs, span, local), BF16),
            jax.ShapeDtypeStruct((seqs, span, local), BF16),
            jax.ShapeDtypeStruct((seqs * heads, span), F32),
            jax.ShapeDtypeStruct((seqs, out_cols), BF16),
        ),
        in_specs=[anywhere, anywhere, anywhere, inside, inside, inside, inside, anywhere],
        out_specs=(anywhere, anywhere, inside, inside),
        scratch_shapes=[
            pltpu.VMEM((seqs, span, width), BF16),
            pltpu.VMEM((width, local), BF16),
            pltpu.VMEM((width, local), BF16),
            pltpu.VMEM(out_weight.shape, BF16),
            pltpu.VMEM((n, m, width), BF16),
            pltpu.VMEM((seqs, n, m, width), BF16),
            pltpu.VMEM((seqs, span, local), BF16),
            pltpu.VMEM((seqs, span, local), BF16),
            pltpu.VMEM((n, m // 4, 128), F32),
            pltpu.VMEM((n, m // 4, 128), F32),
            pltpu.VMEM((seqs * heads, local), BF16),
            pltpu.VMEM((seqs * heads, span), F32),
            pltpu.VMEM((seqs * heads, span), BF16),
            pltpu.VMEM((seqs, local), F32),
            pltpu.VMEM((seqs, local), F32),
            pltpu.VMEM((2 * seqs, 128), F32),
            pltpu.VMEM((n, 2 * seqs, 128), F32),
            pltpu.VMEM((seqs, local), BF16),
            pltpu.VMEM((n, seqs, local), BF16),
            pltpu.VMEM((n + 8, 128), F32),
            pltpu.VMEM((seqs, out_cols), BF16),
            pltpu.VMEM((seqs, out_cols), BF16),
            dma((5,)),
            dma,
            dma((2, GROUPS)),
        ]
        + [dma((n,))] * 10
        + [dma, dma],
        compiler_params=pltpu.CompilerParams(
            collective_id=0, has_side_effects=True, vmem_limit_bytes=60 * 1024 * 1024
        ),
    )(tokens, key_weight, value_weight, gates, new_input, new_query, new_gate, out_weight)
    gate_cache = jnp.swapaxes(gate_cache.reshape(seqs, heads, span), 1, 2)
    return (
        key_cache[:, None],
        value_cache[:, None],
        gate_cache[:, None],
        mixed,
    )


def fits(mesh):
    def holds(tokens, key_weight, value_weight, cum_gate, *rest):
        n = lax.axis_size("sp")
        seqs, span, width = tokens.shape
        heads = cum_gate.shape[2]
        local = key_weight.shape[1]
        m = span // n
        return (
            lax.axis_size("tp") == 2
            and seqs == 2
            and m % 16 == 0
            and m & (m - 1) == 0
            and n % GROUPS == 0
            and n & (n - 1) == 0
            and 4 * seqs * heads == 128
            and local % TILE == 0
            and width % 512 == 0
        )

    def chosen(*arrays):
        return body(*arrays) if holds(*arrays) else plain_body(*arrays)

    return chosen


def solution(mesh):
    placed = (
        P(None, "sp", None),
        P(None, "tp"),
        P(None, "tp"),
        P(None, "sp", "tp"),
        P(),
        P(None, "tp"),
        P(None, "tp"),
        P("tp", "sp"),
    )
    return jax.shard_map(
        fits(mesh),
        mesh=mesh,
        in_specs=placed,
        out_specs=(
            P(None, "sp", None, "tp"),
            P(None, "sp", None, "tp"),
            P(None, "sp", None, "tp"),
            P(None, "sp"),
        ),
        check_vma=False,
    )
```

```python
import functools
import jax
import jax.numpy as jnp
from jax import lax
from jax.experimental import pallas as pl
from jax.experimental.pallas import tpu as pltpu
from jax.sharding import PartitionSpec as P

MESH = pl.DeviceIdType.MESH
F32 = jnp.float32
BF16 = jnp.bfloat16
EXACT = lax.Precision.HIGHEST
GROUPS = 4
TILE = 256


def joined(value, axis, join):
    pieces = jax.tree.map(lambda part: lax.all_gather(part, axis), value)
    head = jax.tree.map(lambda part: part[0], pieces)
    tail = jax.tree.map(lambda part: part[1:], pieces)
    running, _ = lax.scan(lambda running, share: (join(running, share), None), head, tail)
    return running


def combine_parts(first, second):
    highest = jnp.maximum(first[0], second[0])
    first_scale = jnp.exp(first[0] - highest)
    second_scale = jnp.exp(second[0] - highest)
    total = first[1] * first_scale + second[1] * second_scale
    numer = first[2] * first_scale[:, :, None] + second[2] * second_scale[:, :, None]
    return (highest, total, numer)


def plain_body(tokens, key_weight, value_weight, cum_gate, new_input, new_query, new_gate, out_weight):
    local_width = key_weight.shape[1]
    parts = lax.axis_size("sp")
    seq_count, span, width = tokens.shape
    per_peer = span // parts
    flat_rows = tokens.reshape(seq_count * span, width)
    key_local = jnp.dot(flat_rows, key_weight, preferred_element_type=jnp.float32).astype(
        jnp.bfloat16
    )
    value_local = jnp.dot(flat_rows, value_weight, preferred_element_type=jnp.float32).astype(
        jnp.bfloat16
    )
    shaped = (seq_count, per_peer, parts, local_width)
    key_moved, value_moved = (
        lax.all_to_all(key_local.reshape(shaped), "sp", split_axis=2, concat_axis=1, tiled=True),
        lax.all_to_all(value_local.reshape(shaped), "sp", split_axis=2, concat_axis=1, tiled=True),
    )
    key_cache = key_moved.reshape(seq_count, 1, span, local_width)
    value_cache = value_moved.reshape(seq_count, 1, span, local_width)
    head_count = cum_gate.shape[2]
    gate_shaped = cum_gate.reshape(seq_count, per_peer, parts, head_count)
    gate_cache = lax.all_to_all(gate_shaped, "sp", split_axis=2, concat_axis=1, tiled=True).reshape(
        seq_count, 1, span, head_count
    )
    head_size = local_width // head_count
    score_scale = head_size ** (-0.5)
    key_now = jnp.dot(new_input, key_weight, preferred_element_type=jnp.float32).astype(
        jnp.bfloat16
    )
    value_now = jnp.dot(new_input, value_weight, preferred_element_type=jnp.float32).astype(
        jnp.bfloat16
    )
    key_now = key_now.reshape(seq_count, head_count, head_size)
    value_now = value_now.reshape(seq_count, head_count, head_size)
    query_heads = new_query.reshape(seq_count, head_count, head_size)
    key_heads = key_cache.reshape(seq_count, span, head_count, head_size)
    value_heads = value_cache.reshape(seq_count, span, head_count, head_size)
    scores = (
        jnp.einsum("nhd,nlhd->nhl", query_heads, key_heads, preferred_element_type=jnp.float32)
        * score_scale
    )
    scores = (
        scores
        + new_gate[:, :, None]
        - jnp.swapaxes(gate_cache.reshape(seq_count, span, head_count), 1, 2)
    )
    class_top = jnp.max(scores, axis=2)
    expo = jnp.exp(scores - class_top[:, :, None])
    class_total = jnp.sum(expo, axis=2)
    class_num = jnp.einsum(
        "nhl,nlhd->nhd", expo.astype(jnp.bfloat16), value_heads, preferred_element_type=jnp.float32
    )
    cached_top, cached_total, cached_num = joined(
        (class_top, class_total, class_num), "sp", combine_parts
    )
    own_score = (
        jnp.einsum("nhd,nhd->nh", query_heads, key_now, preferred_element_type=jnp.float32)
        * score_scale
    )
    highest = jnp.maximum(cached_top, own_score)
    keep = jnp.exp(cached_top - highest)
    own_expo = jnp.exp(own_score - highest)
    totals = cached_total * keep + own_expo
    own_rounded = lax.optimization_barrier(own_expo.astype(jnp.bfloat16)).astype(jnp.float32)
    numerator = cached_num * keep[:, :, None] + own_rounded[:, :, None] * value_now.astype(
        jnp.float32
    )
    attended = (numerator / totals[:, :, None]).astype(jnp.bfloat16).reshape(seq_count, local_width)
    partial_value = jnp.dot(attended, out_weight, preferred_element_type=jnp.float32)
    partial_value = lax.optimization_barrier(partial_value.astype(jnp.bfloat16)).astype(jnp.float32)
    mixed = lax.psum(partial_value.astype(jnp.bfloat16), "tp")
    return (key_cache, value_cache, gate_cache, mixed)


def iota(shape, axis):
    return lax.broadcasted_iota(jnp.int32, shape, axis)


def dot(a, b, contract=((1,), (0,)), precision=None):
    return lax.dot_general(
        a, b, (contract, ((), ())), precision=precision, preferred_element_type=F32
    )


def one_hot(condition, dtype):
    return jnp.where(condition, 1.0, 0.0).astype(dtype)


def kernel(
    n, m, heads, head_size,
    tokens_ref, wk_ref, wv_ref, gate_in, input_in, query_in, newgate_in, ow_ref,
    kst, vst, gc_ref, mixed_ref,
    gate_ref, input_ref, query_ref, newgate_ref,
    tok, wk, wv, ow, psend, recv, gsend, grecv, qblk, scores, expo,
    know, vnow, stat, statall, num, numall, coef, xsend, xrecv,
    load_sem, own_sem, tok_ss, tok_rs, fwd_ss, fwd_rs, gate_ss, gate_rs,
    stat_ss, stat_rs, num_ss, num_rs, x_ss, x_rs,
):
    me = lax.axis_index("sp")
    t = lax.axis_index("tp")
    other = 1 - t
    seqs, span, width = tokens_ref.shape
    local = wk_ref.shape[1]
    tiles = local // TILE
    per_group = n // GROUPS
    log_m = m.bit_length() - 1
    log_hd = head_size.bit_length() - 1
    scale = head_size ** (-0.5)

    small = [
        pltpu.make_async_copy(gate_in, gate_ref, load_sem.at[5]),
        pltpu.make_async_copy(input_in, input_ref, load_sem.at[6]),
        pltpu.make_async_copy(query_in, query_ref, load_sem.at[7]),
        pltpu.make_async_copy(newgate_in, newgate_ref, load_sem.at[8]),
    ]
    loads = [
        pltpu.make_async_copy(tokens_ref.at[t], tok.at[t], load_sem.at[0]),
        pltpu.make_async_copy(tokens_ref.at[other], tok.at[other], load_sem.at[1]),
        pltpu.make_async_copy(wk_ref, wk, load_sem.at[2]),
        pltpu.make_async_copy(wv_ref, wv, load_sem.at[3]),
        pltpu.make_async_copy(ow_ref, ow, load_sem.at[4]),
    ]
    loads[0].start()

    barrier = pltpu.get_barrier_semaphore()

    def greet(k, carry):
        pl.semaphore_signal(
            barrier, inc=1, device_id=(lax.rem(me + k, n), t), device_id_type=MESH
        )
        return carry

    lax.fori_loop(1, n, greet, 0)
    pl.semaphore_signal(barrier, inc=1, device_id=(me, other), device_id_type=MESH)

    loads[0].wait()
    for load in small + loads[1:]:
        load.start()
    row = iota((span, span), 0)
    col = iota((span, span), 1)
    perm = one_hot(col == (row & (m - 1)) * n + (row >> log_m), BF16)
    for j in range(width // 512):
        cols = slice(j * 512, (j + 1) * 512)
        psend[:, :, cols] = dot(perm, tok[t, :, cols]).astype(BF16).reshape(n, m, 512)

    for load in small:
        load.wait()
    head_of = iota((heads, local), 1) >> log_hd
    mine = head_of == iota((heads, local), 0)
    for b in range(seqs):
        qblk[b * heads : (b + 1) * heads] = jnp.where(
            mine, query_ref[b : b + 1, :].astype(F32), 0.0
        ).astype(BF16)
    scores[...] = jnp.zeros_like(scores)

    pl.semaphore_wait(barrier, n)

    def peer(k):
        far = lax.div(k, per_group)
        near = lax.rem(k, per_group)
        zone = lax.rem(lax.div(me, per_group) + far, GROUPS)
        return zone * per_group + lax.rem(lax.rem(me, per_group) + near, per_group)

    def tok_copy(k, to, source):
        return pltpu.make_async_remote_copy(
            src_ref=psend.at[to], dst_ref=recv.at[t, source],
            send_sem=tok_ss.at[k], recv_sem=tok_rs.at[source],
            device_id=(to, t), device_id_type=MESH,
        )

    def gate_copy(k, to, source):
        return pltpu.make_async_remote_copy(
            src_ref=gsend.at[to], dst_ref=grecv.at[source],
            send_sem=gate_ss.at[k], recv_sem=gate_rs.at[source],
            device_id=(to, t), device_id_type=MESH,
        )

    def stat_copy(k, to, source):
        return pltpu.make_async_remote_copy(
            src_ref=stat, dst_ref=statall.at[source],
            send_sem=stat_ss.at[k], recv_sem=stat_rs.at[source],
            device_id=(to, t), device_id_type=MESH,
        )

    def num_copy(k, to, source):
        return pltpu.make_async_remote_copy(
            src_ref=num, dst_ref=numall.at[source],
            send_sem=num_ss.at[k], recv_sem=num_rs.at[source],
            device_id=(to, t), device_id_type=MESH,
        )

    def forward(held, source, target_batch):
        return pltpu.make_async_remote_copy(
            src_ref=held, dst_ref=recv.at[target_batch, source],
            send_sem=fwd_ss.at[source], recv_sem=fwd_rs.at[source],
            device_id=(me, other), device_id_type=MESH,
        )

    def send_tokens(k, carry):
        tok_copy(k, peer(k), me).start()
        return carry

    def send_gates(k, carry):
        gate_copy(k, peer(k), me).start()
        return carry

    lax.fori_loop(1, per_group, send_tokens, 0)
    for far in FAR_ORDER[:-1]:
        lax.fori_loop(far * per_group, (far + 1) * per_group, send_tokens, 0)
    own_copy = pltpu.make_async_copy(psend.at[me], recv.at[t, me], own_sem)
    own_copy.start()
    forward(psend.at[me], me, t).start()

    quarter = m // 4
    stacked = jnp.concatenate([gate_ref[...]] * 4, axis=0)
    row = iota((span, span), 0)
    col = iota((span, span), 1)
    block_rows = n * quarter
    log_q = quarter.bit_length() - 1
    step_q = row >> (block_rows.bit_length() - 1)
    inner = row & (block_rows - 1)
    place = (step_q * quarter + (inner & (quarter - 1))) * n + (inner >> log_q)
    moved_gate = dot(one_hot(col == place, F32), stacked, ((1,), (1,)), EXACT)
    lanes = seqs * heads
    keep_lane = (iota(moved_gate.shape, 1) // lanes) == (
        iota(moved_gate.shape, 0) >> (block_rows.bit_length() - 1)
    )
    moved_gate = jnp.where(keep_lane, moved_gate, 0.0)
    packed = moved_gate[0:block_rows]
    for q in range(1, 4):
        packed = packed + moved_gate[q * block_rows : (q + 1) * block_rows]
    for r in range(n):
        gsend[r] = packed[r * quarter : (r + 1) * quarter]

    lax.fori_loop(1, n, send_gates, 0)

    loads[1].wait()
    loads[2].wait()

    def key_tile(j, carry):
        cols = pl.ds(pl.multiple_of(j * TILE, TILE), TILE)
        weight = wk[:, cols]
        know[:, cols] = dot(input_ref[...], weight).astype(BF16).astype(F32)
        for b in range(seqs):
            keys = dot(tok[b], weight).astype(BF16)
            rows = slice(b * heads, (b + 1) * heads)
            scores[rows] += dot(qblk[rows, cols], keys, ((1,), (1,)))
        return carry

    lax.fori_loop(0, tiles, key_tile, 0)

    eye = iota((heads, heads), 0) == iota((heads, heads), 1)
    eye_wide = iota((heads, 128), 0) == iota((heads, 128), 1)
    for b in range(seqs):
        rows = slice(b * heads, (b + 1) * heads)
        lift = jnp.sum(jnp.where(eye, newgate_ref[b : b + 1, :], 0.0), axis=1, keepdims=True)
        score = scores[rows] * scale + lift - gate_ref[rows]
        top = jnp.max(score, axis=1, keepdims=True)
        weights = jnp.exp(score - top)
        total = jnp.sum(weights, axis=1, keepdims=True)
        expo[rows] = weights.astype(BF16)
        stat[b : b + 1, :] = jnp.sum(jnp.where(eye_wide, top, 0.0), axis=0, keepdims=True)
        stat[seqs + b : seqs + b + 1, :] = jnp.sum(
            jnp.where(eye_wide, total, 0.0), axis=0, keepdims=True
        )

    loads[3].wait()

    def value_tile(j, carry):
        cols = pl.ds(pl.multiple_of(j * TILE, TILE), TILE)
        weight = wv[:, cols]
        vnow[:, cols] = dot(input_ref[...], weight).astype(BF16).astype(F32)
        held = (iota((heads, TILE), 1) >> log_hd) + j * (TILE // head_size)
        ours = held == iota((heads, TILE), 0)
        sums = []
        for b in range(seqs):
            values = dot(tok[b], weight).astype(BF16)
            full = dot(expo[b * heads : (b + 1) * heads], values)
            sums.append(jnp.sum(jnp.where(ours, full, 0.0), axis=0, keepdims=True))
        num[:, cols] = jnp.concatenate(sums, axis=0).astype(BF16)
        return carry

    lax.fori_loop(0, tiles, value_tile, 0)

    def send_read(k, carry):
        stat_copy(k, peer(k), me).start()
        num_copy(k, peer(k), me).start()
        return carry

    statall[me] = stat[...]
    numall[me] = num[...]
    lax.fori_loop(1, n, send_read, 0)
    last = FAR_ORDER[-1] * per_group
    lax.fori_loop(last, last + per_group, send_tokens, 0)

    def pass_on(far, near_from):
        def step(near, carry):
            source = peer(far * per_group + near)
            tok_copy(0, source, source).wait_recv()
            forward(recv.at[t, source], source, t).start()
            return carry

        lax.fori_loop(near_from, per_group, step, 0)

    def project(far):
        zone = lax.rem(lax.div(me, per_group) + far, GROUPS)
        start = zone * per_group

        def arrived(near, carry):
            forward(recv.at[other, start + near], start + near, other).wait_recv()
            return carry

        lax.fori_loop(0, per_group, arrived, 0)
        rows = pl.ds(pl.multiple_of(start * m, per_group * m), per_group * m)

        def tile(j, carry):
            cols = pl.ds(pl.multiple_of(j * TILE, TILE), TILE)
            block = recv[:, pl.ds(start, per_group)].reshape(seqs * per_group * m, width)
            made = dot(block, wk[:, cols]).astype(BF16)
            kst[:, rows, cols] = made.reshape(seqs, per_group * m, TILE)
            made = dot(block, wv[:, cols]).astype(BF16)
            vst[:, rows, cols] = made.reshape(seqs, per_group * m, TILE)
            return carry

        lax.fori_loop(0, tiles, tile, 0)

    def finish_gates():
        def arrived(k, carry):
            source = peer(k)
            gate_copy(k, source, source).wait_recv()
            return carry

        lax.fori_loop(1, n, arrived, 0)
        grecv[me] = gsend[me]
        held = jnp.concatenate([grecv[s] for s in range(n)], axis=0)
        place_row = iota((block_rows, span), 0)
        target = ((place_row >> log_q) << log_m) + (place_row & (quarter - 1))
        spot = iota((block_rows, span), 1)
        result = None
        for q in range(4):
            part = dot(held, one_hot(spot == target + q * quarter, F32), ((0,), (0,)), EXACT)
            part = part[q * lanes : (q + 1) * lanes]
            result = part if result is None else result + part
        gc_ref[...] = result

    def finish_read():
        def arrived(k, carry):
            source = peer(k)
            stat_copy(k, source, source).wait_recv()
            num_copy(k, source, source).wait_recv()
            return carry

        lax.fori_loop(1, n, arrived, 0)
        loads[4].wait()
        widen = one_hot((iota((128, local), 1) >> log_hd) == iota((128, local), 0), F32)
        own = dot(query_ref[...].astype(F32) * know[...], widen, ((1,), (1,)), EXACT) * scale
        numbers = numall[...].astype(F32)
        attended = []
        for b in range(seqs):
            tops = statall[:, b, :]
            totals = statall[:, seqs + b, :]
            cached_top = jnp.max(tops, axis=0, keepdims=True)
            weight = jnp.exp(tops - cached_top)
            cached_total = jnp.sum(weight * totals, axis=0, keepdims=True)
            own_score = own[b : b + 1]
            highest = jnp.maximum(cached_top, own_score)
            keep = jnp.exp(cached_top - highest)
            own_expo = jnp.exp(own_score - highest)
            total = cached_total * keep + own_expo
            coef[0:n] = weight * (keep / total)
            coef[n : n + 8] = jnp.broadcast_to(own_expo.astype(BF16).astype(F32) / total, (8, 128))
            wide = dot(coef[...], widen, precision=EXACT)
            cached = jnp.sum(numbers[:, b, :] * wide[0:n], axis=0, keepdims=True)
            attended.append(cached + vnow[b : b + 1, :] * wide[n : n + 1])
        attended = jnp.concatenate(attended, axis=0).astype(BF16)
        xsend[...] = dot(attended, ow[...]).astype(BF16)

    own_copy.wait()
    pass_on(0, 1)
    finish_gates()
    project(0)
    for far in FAR_ORDER[:-1]:
        pass_on(far, 0)
        project(far)
    finish_read()
    swap = pltpu.make_async_remote_copy(
        src_ref=xsend, dst_ref=xrecv, send_sem=x_ss, recv_sem=x_rs,
        device_id=(me, other), device_id_type=MESH,
    )
    swap.start()
    pass_on(FAR_ORDER[-1], 0)
    project(FAR_ORDER[-1])
    swap.wait()
    mixed_ref[...] = (xsend[...].astype(F32) + xrecv[...].astype(F32)).astype(BF16)

    def sent(k, carry):
        to = peer(k)
        tok_copy(k, to, me).wait_send()
        gate_copy(k, to, me).wait_send()
        stat_copy(k, to, me).wait_send()
        num_copy(k, to, me).wait_send()
        return carry

    lax.fori_loop(1, n, sent, 0)

    def passed(source, carry):
        forward(recv.at[t, source], source, t).wait_send()
        return carry

    lax.fori_loop(0, n, passed, 0)


FAR_ORDER = (1, 3, 2)


def room(rows, local):
    return 67043328 - 4 * rows * local - 128 * 1024


def body(tokens, key_weight, value_weight, cum_gate, new_input, new_query, new_gate, out_weight):
    n = lax.axis_size("sp")
    seqs, span, width = tokens.shape
    local = key_weight.shape[1]
    heads = cum_gate.shape[2]
    head_size = local // heads
    m = span // n
    out_cols = out_weight.shape[1]
    gates = jnp.swapaxes(cum_gate, 1, 2).reshape(seqs * heads, span)
    far_off = pl.BlockSpec(memory_space=pltpu.HBM)
    inside = pl.BlockSpec(memory_space=pltpu.VMEM)
    dma = pltpu.SemaphoreType.DMA
    key_cache, value_cache, gate_cache, mixed = pl.pallas_call(
        functools.partial(kernel, n, m, heads, head_size),
        out_shape=(
            pltpu.VMEM((seqs, span, local), BF16),
            pltpu.VMEM((seqs, span, local), BF16),
            pltpu.VMEM((seqs * heads, span), F32),
            pltpu.VMEM((seqs, out_cols), BF16),
        ),
        in_specs=[far_off] * 8,
        out_specs=(inside, inside, inside, inside),
        scratch_shapes=[
            pltpu.VMEM((seqs * heads, span), F32),
            pltpu.VMEM(new_input.shape, BF16),
            pltpu.VMEM(new_query.shape, BF16),
            pltpu.VMEM(new_gate.shape, F32),
            pltpu.VMEM((seqs, span, width), BF16),
            pltpu.VMEM((width, local), BF16),
            pltpu.VMEM((width, local), BF16),
            pltpu.VMEM(out_weight.shape, BF16),
            pltpu.VMEM((n, m, width), BF16),
            pltpu.VMEM((seqs, n, m, width), BF16),
            pltpu.VMEM((n, m // 4, 128), F32),
            pltpu.VMEM((n, m // 4, 128), F32),
            pltpu.VMEM((seqs * heads, local), BF16),
            pltpu.VMEM((seqs * heads, span), F32),
            pltpu.VMEM((seqs * heads, span), BF16),
            pltpu.VMEM((seqs, local), F32),
            pltpu.VMEM((seqs, local), F32),
            pltpu.VMEM((2 * seqs, 128), F32),
            pltpu.VMEM((n, 2 * seqs, 128), F32),
            pltpu.VMEM((seqs, local), BF16),
            pltpu.VMEM((n, seqs, local), BF16),
            pltpu.VMEM((n + 8, 128), F32),
            pltpu.VMEM((seqs, out_cols), BF16),
            pltpu.VMEM((seqs, out_cols), BF16),
            dma((9,)),
            dma,
        ]
        + [dma((n,))] * 10
        + [dma, dma],
        compiler_params=pltpu.CompilerParams(
            collective_id=0, has_side_effects=True, vmem_limit_bytes=room(seqs * span, local)
        ),
    )(tokens, key_weight, value_weight, gates, new_input, new_query, new_gate, out_weight)
    gate_cache = jnp.swapaxes(gate_cache.reshape(seqs, heads, span), 1, 2)
    return (
        key_cache[:, None],
        value_cache[:, None],
        gate_cache[:, None],
        mixed,
    )


def fits(mesh):
    def holds(tokens, key_weight, value_weight, cum_gate, *rest):
        n = lax.axis_size("sp")
        seqs, span, width = tokens.shape
        heads = cum_gate.shape[2]
        local = key_weight.shape[1]
        m = span // n
        return (
            lax.axis_size("tp") == 2
            and seqs == 2
            and m % 16 == 0
            and m & (m - 1) == 0
            and n % GROUPS == 0
            and n & (n - 1) == 0
            and 4 * seqs * heads == 128
            and local % TILE == 0
            and width % 512 == 0
        )

    def chosen(*arrays):
        return body(*arrays) if holds(*arrays) else plain_body(*arrays)

    return chosen


def solution(mesh):
    placed = (
        P(None, "sp", None),
        P(None, "tp"),
        P(None, "tp"),
        P(None, "sp", "tp"),
        P(),
        P(None, "tp"),
        P(None, "tp"),
        P("tp", "sp"),
    )
    return jax.shard_map(
        fits(mesh),
        mesh=mesh,
        in_specs=placed,
        out_specs=(
            P(None, "sp", None, "tp"),
            P(None, "sp", None, "tp"),
            P(None, "sp", None, "tp"),
            P(None, "sp"),
        ),
        check_vma=False,
    )
```
